256 devices in a mesh: ep: 16 (over y, x), tp: 16 (over z, core).
Axes of the slice: x: 4, y: 4, z: 8, core: 2. Of those that a mesh axis runs over, the one named last changes fastest.
Arguments:
- queries: bfloat16 [32768, 1024], P('ep', 'tp'), may hold values from -600 to 600
- key_rows: bfloat16 [32768, 128], P('ep'), may hold values from -6 to 6
- value_rows: bfloat16 [32768, 128], P('ep'), may hold values from -48 to 48
- sink_logits: float32 [16], P('tp'), may hold values from 2 to 6
- out_weight: bfloat16 [1024, 2048], P('tp'), may hold values from -0.1875 to 0.1875
- moe_rows: bfloat16 [8192, 2048], P(('ep', 'tp')), may hold values from -6 to 6
- moe_gain: float32 [2048], replicated, may hold values from 0.1 to 1.9
- routes: int32 [8192, 2], P(('ep', 'tp')), may hold values from 0 to 15, all different within a row; in each aligned block of 32 rows (0 to 31, 32 to 63, ...) at most 6 rows name the same one
- route_weight: float32 [8192, 2], P(('ep', 'tp')), may hold values from 0.2 to 1
- gate_weight: bfloat16 [16, 2048, 7168], P('ep', None, 'tp'), may hold values from -0.125 to 0.125
- up_weight: bfloat16 [16, 2048, 7168], P('ep', None, 'tp'), may hold values from -0.125 to 0.125
- down_weight: bfloat16 [16, 7168, 2048], P('ep', 'tp'), may hold values from -0.0625 to 0.0625
Outputs:
- mixer_out: bfloat16 [32768, 2048], P(('ep', 'tp'))
- moe_out: bfloat16 [8192, 2048], P(('ep', 'tp'))
The draws below stay inside these ranges and needn't reach their ends.
Inputs may be any that keep to these rules, and one draw needn't show every extreme that they name: `routes`: in each aligned block of 32 rows (the rows of one device) no expert is named more than 6 times, a bound that some block reaches; each row names 2 different experts.
All inputs are finite; a program needn't handle non-finite values.
Results may differ from the reference program's by a relative error of at most 0.02.
Values may be sent and summed in bfloat16 or wider, within the bound.
A program may use at most 128 MiB of HBM per device.

```python
import math
import jax
import jax.numpy as jnp
import numpy as np
from jax import lax

D = 2048
HEADS = 16
KV_HEADS = 2
HEAD_DIM = 64
WINDOW = 128
FF = 7168
TOP = 2
MOE_DEV = 32
EXPERTS = 16
TOKENS = 32768
MOE_TOKENS = 8192
CAP = 6
N_TP = 16


def draw_queries(key, part):
    base = jax.random.truncated_normal(key, -6.0, 6.0, (TOKENS, HEADS * HEAD_DIM), jnp.float32)
    return base.astype(jnp.bfloat16)


def block_levels(rng, extent, shards, smallest, largest):
    level, own = 1.0, jax.random.fold_in(rng, 6)
    for dim, shards_of in shards:
        draws = jnp.exp(jax.random.uniform(jax.random.fold_in(own, dim), (shards_of,), jnp.float32, smallest / len(shards), largest / len(shards)))
        level = level * jnp.repeat(draws, extent[dim] // shards_of).reshape([-1 if axis == dim else 1 for axis in range(len(extent))])
    return level


def assign_block(own_key, own, number, rows, count, top, most, slope):
    sequence = jax.random.permutation(own_key, count)
    crowded, ordinary = portions_of(count, rows * top, most, slope, True), portions_of(count, rows * top, most, slope, False)
    places = jnp.arange(count)

    def named(tallies, turn):
        used = int((tallies > 0).sum())
        fixed = max(1, used // 4)
        shifted = fixed + (places - fixed + turn * (used - fixed)) % max(1, count - fixed)
        return jnp.zeros((count,), jnp.int32).at[sequence[jnp.where(places < fixed, places, shifted)]].set(jnp.asarray(tallies, jnp.int32))

    tallies = jnp.where(number % 4 == 0, named(crowded, number // 4), named(ordinary, number - number // 4 - 1))
    mixed = jax.random.permutation(jax.random.fold_in(own, 3), count)
    donor, receiver = mixed[0:count // 2 * 2:2], mixed[1:count // 2 * 2:2]
    room = jnp.minimum(tallies[donor] - 1, most - tallies[receiver]) // 2
    room = jnp.where((donor == sequence[0]) | (receiver == sequence[0]) | (tallies[receiver] == 0), 0, jnp.maximum(room, 0))
    shifted = jax.random.randint(jax.random.fold_in(own, 4), (count // 2,), 0, 1 << 20) % (room + 1)
    tallies = tallies.at[donor].add(-shifted).at[receiver].add(shifted)
    members = jnp.searchsorted(jnp.cumsum(tallies), jnp.arange(rows * top), side="right").astype(jnp.int32)
    listing = members.reshape(top, rows).T
    listing = listing[jax.random.permutation(jax.random.fold_in(own, 1), rows)]
    turn = jax.random.randint(jax.random.fold_in(own, 2), (rows, 1), 0, top)
    return jnp.take_along_axis(listing, (jnp.arange(top)[None, :] + turn) % top, axis=1)


def portions_of(amount, total, most, slope, full):
    loads = [(1 << 20) // math.isqrt(standing ** slope) + 1 for standing in range(1, amount + 1)]
    largest = most if full else min(most, max(-(-total // amount), total * loads[0] // sum(loads)))
    least = 1 if total - largest >= amount - 1 else 0
    given, rest = [largest] + [least] * (amount - 1), total - largest - least * (amount - 1)
    while rest > 0:
        free = [i for i in range(1, amount) if given[i] < largest] or [i for i in range(1, amount) if given[i] < most]
        mass, budget = sum([loads[i] for i in free]), rest
        for i in free:
            more = min(most - given[i], max(1, budget * loads[i] // mass), rest)
            given[i] = given[i] + more
            rest = rest - more
    return np.array(given)


def centred(rng, dims, scale, bound, shards=(), kind=jnp.bfloat16):
    level = block_levels(rng, dims, shards, -0.22, 0.18) if shards else 1.0
    drawn = jax.random.normal(rng, dims, jnp.float32) * scale * level
    return jnp.minimum(jnp.maximum(drawn, -bound), bound).astype(kind)


def setup_inputs(seed: int = 0) -> dict:
    seeds = jax.random.split(jax.random.key(seed), 13)
    queries = draw_queries(jax.random.fold_in(seeds[12], 71), 0)
    key_rows = centred(seeds[1], (TOKENS, KV_HEADS * HEAD_DIM), 1.0, 6.0, ((0, 16),))
    value_rows = centred(seeds[2], (TOKENS, KV_HEADS * HEAD_DIM), 8.0, 48.0, ((0, 16),))
    sink_logits = jnp.clip(2.0 + 4.0 * jax.random.uniform(seeds[3], (HEADS,), jnp.float32) ** block_levels(seeds[3], (HEADS,), ((0, 16),), -0.2, 0.2), 2.0, 6.0)
    out_weight = centred(seeds[4], (HEADS * HEAD_DIM, D), (HEADS * HEAD_DIM) ** -0.5, 0.1875, ((0, 16),))
    moe_rows = centred(seeds[5], (MOE_TOKENS, D), 1.0, 6.0, ((0, 256),))
    moe_gain = jnp.clip(1.0 + 0.18 * jax.random.normal(seeds[6], (D,), jnp.float32), 0.1, 1.9)
    routes_keys = jax.random.split(jax.random.fold_in(seeds[7], 1), MOE_TOKENS // MOE_DEV)
    routes_turns = jax.random.permutation(jax.random.fold_in(seeds[7], 3), MOE_TOKENS // MOE_DEV)
    routes = jax.vmap(lambda own, number: assign_block(jax.random.fold_in(seeds[7], 2), own, number, MOE_DEV, EXPERTS, TOP, CAP, 2))(routes_keys, routes_turns).reshape((MOE_TOKENS, TOP))
    route_weight = jnp.clip(0.2 + 0.8 * jax.random.uniform(seeds[8], (MOE_TOKENS, TOP), jnp.float32) ** block_levels(seeds[8], (MOE_TOKENS, TOP), ((0, 256),), -0.2, 0.2), 0.2, 1.0)
    gate_weight = centred(seeds[9], (EXPERTS, D, FF), D ** -0.5, 0.125, ((0, 16), (2, 16)))
    up_weight = centred(seeds[10], (EXPERTS, D, FF), D ** -0.5, 0.125, ((0, 16), (2, 16)))
    down_weight = centred(seeds[11], (EXPERTS, FF, D), FF ** -0.5, 0.0625, ((0, 16), (1, 16)))
    return {"queries": queries, "key_rows": key_rows, "value_rows": value_rows, "sink_logits": sink_logits, "out_weight": out_weight, "moe_rows": moe_rows, "moe_gain": moe_gain, "routes": routes, "route_weight": route_weight, "gate_weight": gate_weight, "up_weight": up_weight, "down_weight": down_weight}


big_negative = -1e+30
norm_eps = 1e-05

def stored_bf16(values):
    return lax.optimization_barrier(values.astype(jnp.bfloat16)).astype(jnp.float32)

def layer_normed(inputs, gain):
    values = inputs.astype(jnp.float32)
    center = values - lax.optimization_barrier(jnp.mean(values, -1, keepdims=True))
    spread = lax.optimization_barrier(jnp.mean(center * center, -1, keepdims=True))
    return (center * lax.rsqrt(spread + norm_eps) * gain).astype(jnp.bfloat16)

def one_head(head_index, queries, key_rows, value_rows, sink_logits):
    total = queries.shape[0]
    blocks = total // WINDOW
    key_head = head_index // (HEADS // KV_HEADS)
    query_cols = lax.dynamic_slice_in_dim(queries, head_index * HEAD_DIM, HEAD_DIM, 1).astype(jnp.float32)
    key_cols = lax.dynamic_slice_in_dim(key_rows, key_head * HEAD_DIM, HEAD_DIM, 1).astype(jnp.float32)
    value_cols = lax.dynamic_slice_in_dim(value_rows, key_head * HEAD_DIM, HEAD_DIM, 1).astype(jnp.float32)
    padding = jnp.zeros((WINDOW, HEAD_DIM), jnp.float32)
    key_ext = jnp.concatenate([padding, key_cols], 0)
    value_ext = jnp.concatenate([padding, value_cols], 0)
    key_blocks = jnp.concatenate([key_ext[:total].reshape(blocks, WINDOW, HEAD_DIM), key_ext[WINDOW:].reshape(blocks, WINDOW, HEAD_DIM)], 1)
    value_blocks = jnp.concatenate([value_ext[:total].reshape(blocks, WINDOW, HEAD_DIM), value_ext[WINDOW:].reshape(blocks, WINDOW, HEAD_DIM)], 1)
    scores = jnp.einsum('nqd,nkd->nqk', query_cols.reshape(blocks, WINDOW, HEAD_DIM), key_blocks) * HEAD_DIM ** (-0.5)
    block_base = jnp.arange(blocks, dtype=jnp.int32)[:, None, None] * WINDOW
    query_pos = block_base + jnp.arange(WINDOW, dtype=jnp.int32)[None, :, None]
    key_pos = block_base - WINDOW + jnp.arange(2 * WINDOW, dtype=jnp.int32)[None, None, :]
    allowed = (key_pos <= query_pos) & (key_pos > query_pos - WINDOW) & (key_pos >= 0)
    masked = jnp.where(allowed, scores, big_negative)
    sink = sink_logits[head_index]
    row_max = jnp.maximum(lax.optimization_barrier(jnp.max(masked, -1)), sink)
    powers = jnp.where(allowed, jnp.exp(masked - row_max[..., None]), 0.0)
    totals = lax.optimization_barrier(jnp.sum(powers, -1)) + jnp.exp(sink - row_max)
    attn_probs = stored_bf16(powers / totals[..., None])
    attended = jnp.einsum('nqk,nkd->nqd', attn_probs, value_blocks)
    return attended.astype(jnp.bfloat16).reshape(total, HEAD_DIM)

def one_expert(inputs):
    expert_rows, gate_mat, up_mat, down_mat = inputs
    gate_val = jnp.dot(expert_rows, gate_mat, preferred_element_type=jnp.float32)
    up_val = jnp.dot(expert_rows, up_mat, preferred_element_type=jnp.float32)
    hidden = (jax.nn.silu(gate_val) * up_val).astype(jnp.bfloat16)
    group_units = FF // N_TP

    def add_group(index, carry):
        first_col = index.astype(jnp.int32) * group_units
        hidden_cols = lax.dynamic_slice_in_dim(hidden, first_col, group_units, 1)
        down_rows = lax.dynamic_slice_in_dim(down_mat, first_col, group_units, 0)
        return carry + stored_bf16(jnp.dot(hidden_cols, down_rows, preferred_element_type=jnp.float32))
    summed = lax.fori_loop(0, N_TP, add_group, jnp.zeros((expert_rows.shape[0], D), jnp.float32))
    return summed.astype(jnp.bfloat16)

def reference(queries, key_rows, value_rows, sink_logits, out_weight, moe_rows, moe_gain, routes, route_weight, gate_weight, up_weight, down_weight):
    total = queries.shape[0]
    per_head = lax.map(lambda index: one_head(index, queries, key_rows, value_rows, sink_logits), jnp.arange(HEADS, dtype=jnp.int32))
    attended = jnp.transpose(per_head, (1, 0, 2)).reshape(total, HEADS * HEAD_DIM)
    group_cols = HEADS // N_TP * HEAD_DIM

    def add_heads(index, carry):
        first_col = index.astype(jnp.int32) * group_cols
        head_cols = lax.dynamic_slice_in_dim(attended, first_col, group_cols, 1)
        proj_rows = lax.dynamic_slice_in_dim(out_weight, first_col, group_cols, 0)
        return carry + stored_bf16(jnp.dot(head_cols, proj_rows, preferred_element_type=jnp.float32))
    mixer_out = lax.fori_loop(0, N_TP, add_heads, jnp.zeros((total, D), jnp.float32)).astype(jnp.bfloat16)
    normed = layer_normed(moe_rows, moe_gain)
    devices = MOE_TOKENS // MOE_DEV
    chosen = routes.reshape(devices, MOE_DEV * TOP).astype(jnp.int32)
    onehot = (chosen[..., None] == jnp.arange(EXPERTS, dtype=jnp.int32)[None, None, :]).astype(jnp.int32)
    earlier_count = jnp.cumsum(onehot, 1) - onehot
    slot_index = lax.optimization_barrier(jnp.sum(earlier_count * onehot, -1)).astype(jnp.int32)
    device_index = jnp.arange(devices, dtype=jnp.int32)[:, None]
    position = ((chosen * devices + device_index) * CAP + slot_index).reshape(-1).astype(jnp.int32)
    token_of = (jnp.arange(MOE_TOKENS * TOP, dtype=jnp.int32) // TOP).astype(jnp.int32)
    buffer = jnp.zeros((EXPERTS * devices * CAP, D), jnp.bfloat16).at[position].set(normed[token_of])
    buffer = buffer.reshape(EXPERTS, devices * CAP, D)
    results = lax.map(one_expert, (buffer, gate_weight, up_weight, down_weight))
    picked = results.reshape(EXPERTS * devices * CAP, D)[position].astype(jnp.float32)
    picked = picked.reshape(MOE_TOKENS, TOP, D)
    moe_out = lax.optimization_barrier(jnp.sum(picked * route_weight[:, :, None], 1)).astype(jnp.bfloat16)
    return (mixer_out, moe_out)
```

```python
import jax
import jax.numpy as jnp
from jax import lax
from jax.experimental import pallas as pl
from jax.experimental.pallas import tpu as pltpu
from jax.sharding import PartitionSpec as P

MESH = pl.DeviceIdType.MESH
F32 = jnp.float32
BF16 = jnp.bfloat16
HEAD_DIM = 64
WINDOW = 128
NORM_EPS = 1e-5
EP = 16
NZ = 8
TPN = 16
CAP = 6
ROWS = 96
HALF = 48
D = 2048
FF = 448
LONG = ((4, 3), (3, 4))


def nt(a, b):
    return lax.dot_general(a, b, (((1,), (1,)), ((), ())), preferred_element_type=F32)


def mm(a, b):
    return jnp.dot(a, b, preferred_element_type=F32)


def iota(shape, dim):
    return lax.broadcasted_iota(jnp.int32, shape, dim)


def wrap(i, n):
    return lax.rem(i + n, n)


def kernel(
    rows_ref,
    gain_ref,
    routes_ref,
    rw_ref,
    sink_ref,
    q_hbm,
    k_hbm,
    v_hbm,
    ow_hbm,
    wg_hbm,
    wu_hbm,
    wd_hbm,
    mix_ref,
    moe_ref,
    wg,
    wu,
    wd,
    qv,
    qsend,
    qrecv,
    sksend,
    skrecv,
    kbuf,
    vbuf,
    kz,
    vz,
    att,
    wr,
    asend,
    arecv,
    agbuf,
    pbuf,
    outbox,
    inbox,
    rs_send,
    rs_recv,
    bsend,
    brecv,
    loc,
    s_a,
    r_a,
    s_b,
    r_b,
    s_q,
    r_q,
    s_k,
    r_k,
    s_h,
    r_h,
    s_wz,
    r_wz,
    s_wp,
    r_wp,
    s_wd,
    r_wd,
    s_ag,
    r_ag,
    s_d,
    r_d,
    s_x,
    r_x,
    s_rs,
    r_rs,
):
    e = lax.axis_index("ep")
    t = lax.axis_index("tp")
    z = t // 2
    c = lax.rem(t, 2)
    right = (e, wrap(z + 1, NZ) * 2 + c)
    left = (e, wrap(z - 1, NZ) * 2 + c)
    partner = (e, z * 2 + 1 - c)
    ring = (right, left)

    def rcopy(src, dst, ss, rs, dev):
        return pltpu.make_async_remote_copy(
            src_ref=src, dst_ref=dst, send_sem=ss, recv_sem=rs, device_id=dev, device_id_type=MESH
        )

    def each(lo, hi, fn):
        def body(j, carry):
            fn(j)
            return carry

        lax.fori_loop(lo, hi, body, 0)

    barrier = pltpu.get_barrier_semaphore()

    def greet(j):
        pl.semaphore_signal(barrier, inc=1, device_id=(wrap(e + j, EP), t), device_id_type=MESH)
        pl.semaphore_signal(barrier, inc=1, device_id=(e, wrap(t + j, TPN)), device_id_type=MESH)

    each(1, EP, greet)

    prev = jnp.maximum(t - 1, 0) * WINDOW
    prev = pl.multiple_of(prev, WINDOW)
    own = pl.multiple_of(t * WINDOW, WINDOW)
    wcol = pl.multiple_of(e * 128, 128)
    zrow = pl.multiple_of(z * HEAD_DIM, HEAD_DIM)
    local = [
        pltpu.make_async_copy(q_hbm, qv, loc.at[0]),
        pltpu.make_async_copy(
            ow_hbm.at[:, pl.ds(wcol, 128)], wr.at[c, e, pl.ds(zrow, HEAD_DIM)], loc.at[1]
        ),
        pltpu.make_async_copy(k_hbm.at[pl.ds(prev, WINDOW)], kbuf.at[0], loc.at[2]),
        pltpu.make_async_copy(k_hbm.at[pl.ds(own, WINDOW)], kbuf.at[1], loc.at[3]),
        pltpu.make_async_copy(v_hbm.at[pl.ds(prev, WINDOW)], vbuf.at[0], loc.at[4]),
        pltpu.make_async_copy(v_hbm.at[pl.ds(own, WINDOW)], vbuf.at[1], loc.at[5]),
        pltpu.make_async_copy(wg_hbm.at[0], wg, loc.at[6]),
        pltpu.make_async_copy(wu_hbm.at[0], wu, loc.at[7]),
        pltpu.make_async_copy(wd_hbm.at[0], wd, loc.at[8]),
    ]
    for cp in local:
        cp.start()

    values = rows_ref[...].astype(F32)
    center = values - jnp.mean(values, -1, keepdims=True)
    spread = jnp.mean(center * center, -1, keepdims=True)
    normed = (center * lax.rsqrt(spread + NORM_EPS) * gain_ref[...]).astype(BF16)
    lane16 = iota((32, 16), 1)
    hit0 = routes_ref[:, 0:1] == lane16
    hit1 = routes_ref[:, 1:2] == lane16
    named = jnp.where(hit0 | hit1, 1.0, 0.0).astype(BF16)
    earlier = jnp.where(iota((32, 32), 1) < iota((32, 32), 0), 1.0, 0.0).astype(BF16)
    slot = mm(earlier, named).astype(BF16)
    expand = jnp.where((iota((256, 16), 0) >> 4) == iota((256, 16), 1), 1.0, 0.0).astype(BF16)
    r32 = iota((256, 32), 0)
    chosen = (nt(expand, named) > 0.5) & (nt(expand, slot) == (r32 & 7).astype(F32))
    first_half = ((r32 >> 3) & 1) == 0
    d0 = jnp.where(chosen & first_half, 1.0, 0.0).astype(BF16)
    d1 = jnp.where(chosen & jnp.logical_not(first_half), 1.0, 0.0).astype(BF16)
    packed = mm(d0, normed[:, : D // 2]) + mm(d1, normed[:, D // 2 :])
    asend[...] = packed.astype(BF16).reshape(EP, 16, D // 2)
    sksend[...] = jnp.broadcast_to(sink_ref[...], (8, 128))

    pl.semaphore_wait(barrier, 2 * (EP - 1))

    def a2a_send(j):
        to = wrap(e + j, EP)
        rcopy(asend.at[to], arecv.at[e], s_a.at[j], r_a.at[j], (to, t)).start()

    def a2a_wait(j):
        frm = wrap(e - j, EP)
        rcopy(asend.at[frm], arecv.at[frm], s_a.at[j], r_a.at[j], (frm, t)).wait_recv()

    each(1, EP, a2a_send)
    arecv[e] = asend[e]

    local[1].wait()

    def wz_copy(j):
        to = (e, wrap(z + j, NZ) * 2 + c)
        ref = wr.at[c, e, pl.ds(zrow, HEAD_DIM)]
        return rcopy(ref, ref, s_wz.at[j], r_wz.at[j], to)

    def wz_wait(j):
        frm = pl.multiple_of(wrap(z - j, NZ) * HEAD_DIM, HEAD_DIM)
        ref = wr.at[c, e, pl.ds(frm, HEAD_DIM)]
        rcopy(ref, ref, s_wz.at[j], r_wz.at[j], right).wait_recv()

    each(1, NZ, lambda j: wz_copy(j).start())

    local[0].wait()

    def pack(j):
        lo = qv[pl.ds(pl.multiple_of(j * 128, 128), 64), :]
        hi = qv[pl.ds(pl.multiple_of(j * 128 + 64, 64), 64), :]
        qsend[j] = jnp.concatenate([lo, hi], axis=1)

    each(0, TPN, pack)

    def q_send(j):
        to = wrap(t + j, TPN)
        rcopy(qsend.at[to], qrecv.at[t], s_q.at[j], r_q.at[j], (e, to)).start()
        rcopy(sksend, skrecv.at[t], s_k.at[j], r_k.at[j], (e, to)).start()

    def q_wait(j):
        frm = wrap(t - j, TPN)
        rcopy(qsend.at[frm], qrecv.at[frm], s_q.at[j], r_q.at[j], (e, frm)).wait_recv()
        rcopy(sksend, skrecv.at[frm], s_k.at[j], r_k.at[j], (e, frm)).wait_recv()

    each(1, TPN, q_send)
    qrecv[t] = qsend[t]
    skrecv[t] = sksend[...]
    after = (wrap(e + 1, EP), t)
    halo = [
        rcopy(k_hbm.at[pl.ds((TPN - 1) * WINDOW, WINDOW)], kbuf.at[2], s_h.at[0], r_h.at[0], after),
        rcopy(v_hbm.at[pl.ds((TPN - 1) * WINDOW, WINDOW)], vbuf.at[2], s_h.at[1], r_h.at[1], after),
    ]
    for cp in halo:
        cp.start()

    each(1, EP, a2a_wait)
    r96 = iota((ROWS, 256), 0)
    source = (r96 * 43) >> 8
    base = source * 16 + (r96 - source * CAP)
    arrived = arecv[...].reshape(256, D // 2)
    for h in range(2):
        pick = jnp.where(iota((ROWS, 256), 1) == base + h * 8, 1.0, 0.0).astype(BF16)
        agbuf[t, :, h * (D // 2) : (h + 1) * (D // 2)] = mm(pick, arrived).astype(BF16)

    def chip(direction, k):
        return wrap(z - k if direction == 0 else z + k, NZ)

    def block(zb, core, h):
        return agbuf.at[zb * 2 + core, pl.ds(h * HALF, HALF)]

    def ag_send(direction, k, h):
        ref = block(chip(direction, k - 1), c, h)
        return rcopy(
            ref,
            ref,
            s_ag.at[direction, k - 1, h],
            r_ag.at[direction, k - 1, h],
            ring[direction],
        )

    def ag_wait(direction, k, h):
        ref = block(chip(direction, k), c, h)
        rcopy(
            ref,
            ref,
            s_ag.at[direction, k - 1, h],
            r_ag.at[direction, k - 1, h],
            ring[direction],
        ).wait_recv()

    def d_send(slot_no, zb, h):
        ref = block(zb, c, h)
        return rcopy(ref, ref, s_d.at[slot_no, h], r_d.at[slot_no, h], partner)

    def d_wait(slot_no, zb, h):
        ref = block(zb, 1 - c, h)
        rcopy(ref, ref, s_d.at[slot_no, h], r_d.at[slot_no, h], partner).wait_recv()

    sends = []

    def go(copy):
        copy.start()
        sends.append(copy)

    for h in range(2):
        for direction in range(2):
            go(ag_send(direction, 1, h))
    for h in range(2):
        go(d_send(0, z, h))

    def x_copy(slot_no, zb):
        return rcopy(outbox.at[zb], inbox.at[zb], s_x.at[slot_no], r_x.at[slot_no], partner)

    def compute(zb, slot_no):
        x = jnp.concatenate([agbuf[zb * 2 + c], agbuf[zb * 2 + 1 - c]], axis=0)
        gate = mm(x, wg[...])
        up = mm(x, wu[...])
        hidden = (gate / (1.0 + jnp.exp(-gate)) * up).astype(BF16)
        for col in range(0, D, 512):
            part = mm(hidden, wd[:, col : col + 512])
            pbuf[zb, :, col : col + 512] = part[:ROWS]
            outbox[zb, :, col : col + 512] = part[ROWS:].astype(BF16)
        x_copy(slot_no, zb).start()

    def ring_step(k, h):
        for direction in range(2):
            if k <= LONG[direction][h]:
                ag_wait(direction, k, h)
                if k < LONG[direction][h]:
                    go(ag_send(direction, k + 1, h))
                go(d_send(direction * 4 + k, chip(direction, k), h))

    def event(k):
        for direction in range(2):
            for h in range(2):
                d_wait(direction * 4 + k, chip(direction, k), h)

        def one(i, carry):
            zb = wrap(z - k + 2 * k * i, NZ)
            compute(zb, i * 4 + k)
            return carry

        lax.fori_loop(0, 2, one, 0)

    for cp in local[6:]:
        cp.wait()
    for h in range(2):
        d_wait(0, z, h)
    compute(z, 0)
    each(1, NZ, wz_wait)

    def wp_copy(j):
        to = (wrap(e + j, EP), t)
        return rcopy(wr.at[c, e], wr.at[c, e], s_wp.at[j], r_wp.at[j], to)

    def wp_wait(j):
        frm = wrap(e - j, EP)
        rcopy(wr.at[c, frm], wr.at[c, frm], s_wp.at[j], r_wp.at[j], (frm, t)).wait_recv()

    each(1, EP, lambda j: wp_copy(j).start())

    def prepare_attention():
        for cp in local[2:6]:
            cp.wait()
        for cp in halo:
            cp.wait_recv()
        each(1, TPN, q_wait)
        low = iota((WINDOW, 128), 1) < HEAD_DIM
        for buf, out in ((kbuf, kz), (vbuf, vz)):
            for part in range(2):
                if part == 0:
                    full = jnp.where(t == 0, buf[2].astype(F32), buf[0].astype(F32))
                else:
                    full = buf[1].astype(F32)
                turned = pltpu.roll(full, HEAD_DIM, 1)
                at = pl.ds(part * WINDOW, WINDOW)
                out[0, 0, at] = jnp.where(low, full, 0.0).astype(BF16)
                out[0, 1, at] = jnp.where(low, 0.0, turned).astype(BF16)
                out[1, 0, at] = jnp.where(low, turned, 0.0).astype(BF16)
                out[1, 1, at] = jnp.where(low, 0.0, full).astype(BF16)

    def attend(j):
        core, pair = lax.rem(j, 2), j // 2
        group = j // 4
        token = iota((WINDOW, 2 * WINDOW), 0)
        key = iota((WINDOW, 2 * WINDOW), 1)
        begin = jnp.where((e == 0) & (t == 0), WINDOW, 0)
        allowed = (key > token) & (key <= token + WINDOW) & (key >= begin)
        total = None
        for i in range(2):
            head = pair * 4 + 2 * i + core
            q2 = qrecv[head]
            scores = jnp.concatenate([nt(q2, kz[group, 0]), nt(q2, kz[group, 1])], axis=0)
            masked = jnp.where(allowed, scores * HEAD_DIM**-0.5, -1e30)
            sink = skrecv[head][0:1, 0:1]
            row_max = jnp.maximum(jnp.max(masked, -1, keepdims=True), sink)
            powers = jnp.where(allowed, jnp.exp(masked - row_max), 0.0)
            sums = jnp.sum(powers, -1, keepdims=True) + jnp.exp(sink - row_max)
            probs = (powers / sums).astype(BF16)
            piece = mm(probs, vz[group, i])
            total = piece if total is None else total + piece
        att[j] = total.astype(BF16)

    ring_step(1, 0)
    prepare_attention()
    ring_step(1, 1)
    event(1)
    ring_step(2, 0)
    each(0, 4, attend)
    ring_step(2, 1)
    event(2)
    ring_step(3, 0)
    each(4, 8, attend)
    ring_step(3, 1)
    event(3)

    def x_wait(slot_no, zb):
        x_copy(slot_no, zb).wait_recv()

    def pair_sum(zb, h):
        at = pl.ds(h * HALF, HALF)
        return pbuf[zb, at] + inbox[zb, at].astype(F32)

    def rs_copy(direction, k, h):
        return rcopy(
            rs_send.at[direction, k - 1, h],
            rs_recv.at[direction, k - 1, h],
            s_rs.at[direction, k - 1, h],
            r_rs.at[direction, k - 1, h],
            ring[direction],
        )

    def rs_go(direction, k, h):
        away = LONG[direction][h] + 1 - k
        value = pair_sum(wrap(z + away if direction == 0 else z - away, NZ), h)
        if k > 1:
            value = value + rs_recv[direction, k - 2, h].astype(F32)
        rs_send[direction, k - 1, h] = value.astype(BF16)
        go(rs_copy(direction, k, h))

    x_wait(0, z)
    for k in range(1, 4):
        for direction in range(2):
            x_wait(direction * 4 + k, chip(direction, k))
    rs_go(0, 1, 1)
    rs_go(1, 1, 0)

    ag_wait(0, 4, 0)
    go(d_send(4, chip(0, 4), 0))
    ag_wait(1, 4, 1)
    go(d_send(8, chip(1, 4), 1))
    d_wait(4, chip(0, 4), 0)
    d_wait(8, chip(1, 4), 1)
    compute(chip(0, 4), 4)
    x_wait(4, chip(0, 4))
    rs_go(0, 1, 0)
    rs_go(1, 1, 1)

    each(1, EP, wp_wait)
    wd_copy = rcopy(wr.at[c], wr.at[c], s_wd, r_wd, partner)
    wd_copy.start()

    def project(lo, hi):
        a0 = jnp.concatenate([att[2 * i] for i in range(4)], axis=1)
        a1 = jnp.concatenate([att[2 * i + 1] for i in range(4)], axis=1)
        for i in range(lo, hi):
            out = mm(a0, wr[0, i]) + mm(a1, wr[1, i])
            mix_ref[:, i * 128 : (i + 1) * 128] = out.astype(BF16)

    def rs_step(k):
        for first in (True, False):
            for direction in range(2):
                h = 1 - direction if first else direction
                long = LONG[direction][h]
                if k <= long:
                    rs_copy(direction, k, h).wait_recv()
                    if k < long:
                        rs_go(direction, k + 1, h)

    rs_step(1)
    rcopy(wr.at[1 - c], wr.at[1 - c], s_wd, r_wd, partner).wait_recv()
    project(0, 8)
    rs_step(2)
    project(8, 16)
    rs_step(3)
    rs_step(4)

    halves = []
    for h in range(2):
        value = pair_sum(z, h)
        for direction in range(2):
            value = value + rs_recv[direction, LONG[direction][h] - 1, h].astype(F32)
        halves.append(value.astype(BF16))
    final = jnp.concatenate(halves, axis=0)
    rr = iota((256, ROWS), 0)
    want = (rr >> 4) * CAP + (rr & 7)
    good = (iota((256, ROWS), 1) == want) & ((rr & 7) < CAP)
    low_half = ((rr >> 3) & 1) == 0
    e0 = jnp.where(good & low_half, 1.0, 0.0).astype(BF16)
    e1 = jnp.where(good & jnp.logical_not(low_half), 1.0, 0.0).astype(BF16)
    spread_out = mm(e0, final[:, : D // 2]) + mm(e1, final[:, D // 2 :])
    bsend[...] = spread_out.astype(BF16).reshape(EP, 16, D // 2)

    def b_send(j):
        to = wrap(e + j, EP)
        rcopy(bsend.at[to], brecv.at[e], s_b.at[j], r_b.at[j], (to, t)).start()

    def b_wait(j):
        frm = wrap(e - j, EP)
        rcopy(bsend.at[frm], brecv.at[frm], s_b.at[j], r_b.at[j], (frm, t)).wait_recv()

    each(1, EP, b_send)
    brecv[e] = bsend[e]

    weight = jnp.where(hit0, rw_ref[:, 0:1], 0.0) + jnp.where(hit1, rw_ref[:, 1:2], 0.0)
    w_hi = weight.astype(BF16)
    w_lo = (weight - w_hi.astype(F32)).astype(BF16)
    lane = iota((32, 256), 1)
    mine = (nt(named, expand) > 0.5) & (nt(slot, expand) == (lane & 7).astype(F32))
    first_lane = ((lane >> 3) & 1) == 0
    hi_all = nt(w_hi, expand)
    lo_all = nt(w_lo, expand)
    each(1, EP, b_wait)
    back = brecv[...].reshape(256, D // 2)
    for h in range(2):
        keep = mine & (first_lane if h == 0 else jnp.logical_not(first_lane))
        out = mm(jnp.where(keep, hi_all, 0.0).astype(BF16), back)
        out = out + mm(jnp.where(keep, lo_all, 0.0).astype(BF16), back)
        moe_ref[:, h * (D // 2) : (h + 1) * (D // 2)] = out.astype(BF16)

    def drain(j):
        rcopy(asend.at[j], arecv.at[j], s_a.at[j], r_a.at[j], right).wait_send()
        rcopy(bsend.at[j], brecv.at[j], s_b.at[j], r_b.at[j], right).wait_send()
        rcopy(qsend.at[j], qrecv.at[j], s_q.at[j], r_q.at[j], right).wait_send()
        rcopy(sksend, skrecv.at[j], s_k.at[j], r_k.at[j], right).wait_send()
        wp_copy(j).wait_send()

    each(1, EP, drain)
    each(1, NZ, lambda j: wz_copy(j).wait_send())
    for cp in halo:
        cp.wait_send()
    wd_copy.wait_send()
    for cp in sends:
        cp.wait_send()
    x_copy(0, z).wait_send()
    for k in range(1, 4):
        for direction in range(2):
            x_copy(direction * 4 + k, chip(direction, k)).wait_send()
    x_copy(4, chip(0, 4)).wait_send()


def body(
    queries,
    key_rows,
    value_rows,
    sink_logits,
    out_weight,
    moe_rows,
    moe_gain,
    routes,
    route_weight,
    gate_weight,
    up_weight,
    down_weight,
):
    vm = pl.BlockSpec(memory_space=pltpu.VMEM)
    hbm = pl.BlockSpec(memory_space=pl.ANY)
    dma = pltpu.SemaphoreType.DMA
    half = D // 2
    return pl.pallas_call(
        kernel,
        out_shape=(
            jax.ShapeDtypeStruct((WINDOW, D), BF16),
            jax.ShapeDtypeStruct((32, D), BF16),
        ),
        in_specs=[vm] * 5 + [hbm] * 7,
        out_specs=(vm, vm),
        scratch_shapes=[
            pltpu.VMEM((D, FF), BF16),
            pltpu.VMEM((D, FF), BF16),
            pltpu.VMEM((FF, D), BF16),
            pltpu.VMEM((TPN * WINDOW, HEAD_DIM), BF16),
            pltpu.VMEM((TPN, 64, 128), BF16),
            pltpu.VMEM((TPN, 64, 128), BF16),
            pltpu.VMEM((8, 128), F32),
            pltpu.VMEM((TPN, 8, 128), F32),
            pltpu.VMEM((3, WINDOW, 128), BF16),
            pltpu.VMEM((3, WINDOW, 128), BF16),
            pltpu.VMEM((2, 2, 2 * WINDOW, 128), BF16),
            pltpu.VMEM((2, 2, 2 * WINDOW, 128), BF16),
            pltpu.VMEM((8, WINDOW, 128), BF16),
            pltpu.VMEM((2, EP, NZ * HEAD_DIM, 128), BF16),
            pltpu.VMEM((EP, 16, half), BF16),
            pltpu.VMEM((EP, 16, half), BF16),
            pltpu.VMEM((TPN, ROWS, D), BF16),
            pltpu.VMEM((NZ, ROWS, D), F32),
            pltpu.VMEM((NZ, ROWS, D), BF16),
            pltpu.VMEM((NZ, ROWS, D), BF16),
            pltpu.VMEM((2, 4, 2, HALF, D), BF16),
            pltpu.VMEM((2, 4, 2, HALF, D), BF16),
            pltpu.VMEM((EP, 16, half), BF16),
            pltpu.VMEM((EP, 16, half), BF16),
            dma((9,)),
            dma((EP,)),
            dma((EP,)),
            dma((EP,)),
            dma((EP,)),
            dma((TPN,)),
            dma((TPN,)),
            dma((TPN,)),
            dma((TPN,)),
            dma((2,)),
            dma((2,)),
            dma((NZ,)),
            dma((NZ,)),
            dma((EP,)),
            dma((EP,)),
            dma,
            dma,
            dma((2, 4, 2)),
            dma((2, 4, 2)),
            dma((9, 2)),
            dma((9, 2)),
            dma((8,)),
            dma((8,)),
            dma((2, 4, 2)),
            dma((2, 4, 2)),
        ],
        compiler_params=pltpu.CompilerParams(
            collective_id=0, has_side_effects=True, vmem_limit_bytes=60 * 1024 * 1024
        ),
    )(
        moe_rows,
        moe_gain.reshape(1, D),
        routes,
        route_weight,
        sink_logits.reshape(1, 1),
        queries,
        key_rows,
        value_rows,
        out_weight,
        gate_weight,
        up_weight,
        down_weight,
    )


def solution(mesh):
    in_specs = (
        P("ep", "tp"),
        P("ep", None),
        P("ep", None),
        P("tp"),
        P("tp", None),
        P(("ep", "tp"), None),
        P(),
        P(("ep", "tp"), None),
        P(("ep", "tp"), None),
        P("ep", None, "tp"),
        P("ep", None, "tp"),
        P("ep", "tp", None),
    )
    out_specs = (P(("ep", "tp"), None), P(("ep", "tp"), None))
    return jax.shard_map(body, mesh=mesh, in_specs=in_specs, out_specs=out_specs, check_vma=False)
```

```python
import jax
import jax.numpy as jnp
from jax import lax
from jax.experimental import pallas as pl
from jax.experimental.pallas import tpu as pltpu
from jax.sharding import PartitionSpec as P

MESH = pl.DeviceIdType.MESH
F32 = jnp.float32
BF16 = jnp.bfloat16
HEAD_DIM = 64
WINDOW = 128
NORM_EPS = 1e-5
EP = 16
NZ = 8
TPN = 16
ROWS = 96
HALF = 48
D = 2048
FF = 448
WIDE = D // 2
QUARTER = D // 4
NARROW = D // 2
LONG = ((4, 3), (3, 4))


def nt(a, b):
    return lax.dot_general(a, b, (((1,), (1,)), ((), ())), preferred_element_type=F32)


def mm(a, b):
    return jnp.dot(a, b, preferred_element_type=F32)


def iota(shape, dim):
    return lax.broadcasted_iota(jnp.int32, shape, dim)


def wrap(i, n):
    return lax.rem(i + n, n)


def kernel(
    rows_hbm,
    gain_hbm,
    routes_hbm,
    rw_hbm,
    sink_hbm,
    q_hbm,
    k_hbm,
    v_hbm,
    ow_hbm,
    wg_hbm,
    wu_hbm,
    wd_hbm,
    mix_ref,
    moe_ref,
    rows_ref,
    gain_ref,
    routes_ref,
    rw_ref,
    sink_ref,
    wg,
    wu,
    wd,
    qv,
    qz,
    sksend,
    skrecv,
    kbuf,
    vbuf,
    kf,
    vt,
    att,
    proj,
    wr,
    asend,
    arecv,
    agbuf,
    pbuf,
    outbox,
    inbox,
    rs_send,
    rs_recv,
    bsend,
    brecv,
    loc,
    q_sem,
    s_a,
    r_a,
    s_b,
    r_b,
    s_q,
    r_q,
    s_k,
    r_k,
    s_h,
    r_h,
    s_wz,
    r_wz,
    s_wp,
    r_wp,
    s_wd,
    r_wd,
    s_ag,
    r_ag,
    s_o,
    r_o,
    s_d,
    r_d,
    s_x,
    r_x,
    s_rs,
    r_rs,
):
    e = lax.axis_index("ep")
    t = lax.axis_index("tp")
    z = t // 2
    c = lax.rem(t, 2)
    right = (e, wrap(z + 1, NZ) * 2 + c)
    left = (e, wrap(z - 1, NZ) * 2 + c)
    partner = (e, z * 2 + 1 - c)
    ring = (right, left)

    def rcopy(src, dst, ss, rs, dev):
        return pltpu.make_async_remote_copy(
            src_ref=src, dst_ref=dst, send_sem=ss, recv_sem=rs, device_id=dev, device_id_type=MESH
        )

    def each(lo, hi, fn):
        def body(j, carry):
            fn(j)
            return carry

        lax.fori_loop(lo, hi, body, 0)

    first = [
        pltpu.make_async_copy(src, dst, loc.at[9 + i])
        for i, (src, dst) in enumerate(
            (
                (rows_hbm, rows_ref),
                (gain_hbm, gain_ref),
                (routes_hbm, routes_ref),
                (rw_hbm, rw_ref),
                (sink_hbm, sink_ref),
            )
        )
    ]
    for cp in first:
        cp.start()

    barrier = pltpu.get_barrier_semaphore()

    def greet(j):
        pl.semaphore_signal(barrier, inc=1, device_id=(wrap(e + j, EP), t), device_id_type=MESH)
        pl.semaphore_signal(barrier, inc=1, device_id=(e, wrap(t + j, TPN)), device_id_type=MESH)

    each(1, EP, greet)

    prev = jnp.maximum(t - 1, 0) * WINDOW
    prev = pl.multiple_of(prev, WINDOW)
    own = pl.multiple_of(t * WINDOW, WINDOW)
    wcol = pl.multiple_of(e * 128, 128)
    zrow = pl.multiple_of(z * HEAD_DIM, HEAD_DIM)
    group_row = pl.multiple_of((t // 8) * HEAD_DIM, HEAD_DIM)
    local = [
        pltpu.make_async_copy(
            q_hbm.at[:, pl.ds(own, WINDOW)],
            qz.at[t, pl.ds(group_row, HEAD_DIM)],
            loc.at[0],
        ),
        pltpu.make_async_copy(
            ow_hbm.at[:, pl.ds(wcol, 128)], wr.at[c, e, pl.ds(zrow, HEAD_DIM)], loc.at[1]
        ),
        pltpu.make_async_copy(k_hbm.at[pl.ds(prev, WINDOW)], kbuf.at[0], loc.at[2]),
        pltpu.make_async_copy(k_hbm.at[pl.ds(own, WINDOW)], kbuf.at[1], loc.at[3]),
        pltpu.make_async_copy(v_hbm.at[pl.ds(prev, WINDOW)], vbuf.at[0], loc.at[4]),
        pltpu.make_async_copy(v_hbm.at[pl.ds(own, WINDOW)], vbuf.at[1], loc.at[5]),
        pltpu.make_async_copy(wg_hbm.at[0], wg, loc.at[6]),
        pltpu.make_async_copy(wu_hbm.at[0], wu, loc.at[7]),
        pltpu.make_async_copy(wd_hbm.at[0], wd, loc.at[8]),
    ]
    for cp in local:
        cp.start()

    def q_load(j):
        cols = pl.ds(pl.multiple_of(j * WINDOW, WINDOW), WINDOW)
        pltpu.make_async_copy(q_hbm.at[:, cols], qv.at[j], q_sem).start()

    each(0, TPN, q_load)

    for cp in first:
        cp.wait()
    values = rows_ref[...].astype(F32)
    center = values - jnp.mean(values, -1, keepdims=True)
    spread = jnp.mean(center * center, -1, keepdims=True)
    normed = (center * lax.rsqrt(spread + NORM_EPS) * gain_ref[...]).astype(BF16)
    expert = iota((16, 32), 0)
    hit0 = routes_ref[0:1, :] == expert
    hit1 = routes_ref[1:2, :] == expert
    named = jnp.where(hit0 | hit1, 1.0, 0.0).astype(BF16)
    earlier = jnp.where(iota((32, 32), 0) < iota((32, 32), 1), 1.0, 0.0).astype(BF16)
    slot = mm(named, earlier).astype(BF16)
    expand = jnp.where((iota((256, 16), 0) >> 4) == iota((256, 16), 1), 1.0, 0.0).astype(BF16)
    r32 = iota((256, 32), 0)
    s32 = r32 & 3
    q32 = (r32 >> 2) & 3
    named_rows = mm(expand, named) > 0.5
    slot_rows = mm(expand, slot)
    chosen = []
    for h in range(2):
        chosen.append(named_rows & (s32 < 3) & (slot_rows == (s32 + 3 * h).astype(F32)))
        packed = None
        for q in range(4):
            take = jnp.where(chosen[h] & (q32 == q), 1.0, 0.0).astype(BF16)
            piece = mm(take, normed[:, q * QUARTER : (q + 1) * QUARTER])
            packed = piece if packed is None else packed + piece
        asend[h] = packed.astype(BF16).reshape(EP, 16, QUARTER)
    sksend[...] = jnp.broadcast_to(sink_ref[...], (8, 128))
    for head in range(TPN):
        unused = (1 - head // 8) * HEAD_DIM
        qz[head, unused : unused + HEAD_DIM] = jnp.zeros((HEAD_DIM, WINDOW), BF16)

    pl.semaphore_wait(barrier, 2 * (EP - 1))

    def a_copy(h, to, frm):
        return rcopy(asend.at[h, to], arecv.at[h, frm], s_a.at[h], r_a.at[h], (to, t))

    def a_send(h, j):
        to = wrap(e + j, EP)
        a_copy(h, to, e).start()

    def a_all(h):
        rest = slice(0, EP - 1)
        return rcopy(asend.at[h, rest], arecv.at[h, rest], s_a.at[h], r_a.at[h], right)

    for h in range(2):
        each(1, EP, lambda j: a_send(h, j))
    for h in range(2):
        arecv[h, e] = asend[h, e]

    local[1].wait()

    def wz_copy(direction, k):
        zb = wrap(z - k + 1 if direction == 0 else z + k - 1, NZ)
        ref = wr.at[c, e, pl.ds(pl.multiple_of(zb * HEAD_DIM, HEAD_DIM), HEAD_DIM)]
        return rcopy(ref, ref, s_wz, r_wz.at[direction, k - 1], ring[direction])

    def wz_step(k):
        for direction in range(2):
            if k <= 4 - direction:
                zb = wrap(z - k if direction == 0 else z + k, NZ)
                ref = wr.at[c, e, pl.ds(pl.multiple_of(zb * HEAD_DIM, HEAD_DIM), HEAD_DIM)]
                rcopy(ref, ref, s_wz, r_wz.at[direction, k - 1], right).wait_recv()
                if k < 4 - direction:
                    wz_copy(direction, k + 1).start()

    for direction in range(2):
        wz_copy(direction, 1).start()

    def q_copy(to, frm):
        rows = pl.ds(pl.multiple_of((frm // 8) * HEAD_DIM, HEAD_DIM), HEAD_DIM)
        return rcopy(qv.at[to], qz.at[frm, rows], s_q, r_q, (e, to))

    def q_send(j):
        to = wrap(t + j, TPN)
        q_copy(to, t).start()
        rcopy(sksend, skrecv.at[t], s_k, r_k, (e, to)).start()

    def q_all():
        ref = qz.at[pl.ds(0, TPN - 1), pl.ds(0, HEAD_DIM)]
        return rcopy(ref, ref, s_q, r_q, right)

    def k_all():
        ref = skrecv.at[pl.ds(0, TPN - 1)]
        return rcopy(ref, ref, s_k, r_k, right)

    pltpu.make_async_copy(qv, qv, q_sem).wait()
    each(1, TPN, q_send)
    skrecv[t] = sksend[...]
    after = (wrap(e + 1, EP), t)
    halo = [
        rcopy(k_hbm.at[pl.ds((TPN - 1) * WINDOW, WINDOW)], kbuf.at[2], s_h.at[0], r_h.at[0], after),
        rcopy(v_hbm.at[pl.ds((TPN - 1) * WINDOW, WINDOW)], vbuf.at[2], s_h.at[1], r_h.at[1], after),
    ]
    for cp in halo:
        cp.start()

    def compact(h):
        r48 = iota((HALF, 256), 0)
        source = (r48 * 43) >> 7
        base = source * 16 + (r48 - source * 3)
        lane = iota((HALF, 256), 1)
        arrived = arecv[h].reshape(256, QUARTER)
        for q in range(4):
            pick = jnp.where(lane == base + q * 4, 1.0, 0.0).astype(BF16)
            agbuf[t, h * HALF : (h + 1) * HALF, q * QUARTER : (q + 1) * QUARTER] = mm(
                pick, arrived
            ).astype(BF16)

    def chip(direction, k):
        return wrap(z - k if direction == 0 else z + k, NZ)

    def half_block(zb, core, h):
        return agbuf.at[zb * 2 + core, pl.ds(h * HALF, HALF)]

    def piece_of(zb, core, h, col):
        cols = pl.ds(0, NARROW) if col == 0 else pl.ds(NARROW, D - NARROW)
        return agbuf.at[zb * 2 + core, pl.ds(h * HALF, HALF), cols]

    def ag_copy(direction, k, h, col, zb):
        ref = piece_of(zb, c, h, col)
        return rcopy(
            ref,
            ref,
            s_ag,
            r_ag.at[direction, k - 1, h, col],
            ring[direction],
        )

    def d_copy(direction, k, h, col, core):
        ref = piece_of(chip(direction, k), core, h, col)
        return rcopy(
            ref,
            ref,
            s_d,
            r_d.at[direction, k - 1, h, col],
            partner,
        )

    def o_copy(h, core):
        ref = half_block(z, core, h)
        return rcopy(ref, ref, s_o, r_o.at[h], partner)

    def launch(h):
        a_all(h).wait_recv()
        compact(h)
        for col in range(2):
            for direction in range(2):
                ag_copy(direction, 1, h, col, z).start()
        o_copy(h, c).start()

    def x_copy(zb, h):
        at = pl.ds(h * HALF, HALF)
        return rcopy(outbox.at[zb, at], inbox.at[zb, at], s_x, r_x.at[zb, h], partner)

    def compute(parts):
        ats = [slice(h * HALF, (h + 1) * HALF) for _, h in parts]
        x = jnp.concatenate(
            [agbuf[zb * 2 + core, at] for core in (c, 1 - c) for (zb, _), at in zip(parts, ats)],
            axis=0,
        )
        gate = nt(x, wg[...])
        up = nt(x, wu[...])
        hidden = (gate / (1.0 + jnp.exp(-gate)) * up).astype(BF16)
        for col in range(0, D, 512):
            part = mm(hidden, wd[:, col : col + 512])
            for i, ((zb, _), at) in enumerate(zip(parts, ats)):
                other = (len(parts) + i) * HALF
                pbuf[zb, at, col : col + 512] = part[i * HALF : (i + 1) * HALF]
                outbox[zb, at, col : col + 512] = part[other : other + HALF].astype(BF16)
        for zb, h in parts:
            x_copy(zb, h).start()

    def arrival(k, h, long):
        for direction in range(2):
            col = direction if long else 1 - direction
            ag_copy(direction, k, h, col, chip(direction, k)).wait_recv()
            if k < LONG[direction][col]:
                ag_copy(direction, k + 1, h, col, chip(direction, k)).start()
            d_copy(direction, k, h, col, c).start()

    def event_wait(k, h):
        for col in range(2):
            for direction in range(2):
                if k <= LONG[direction][col]:
                    d_copy(direction, k, h, col, 1 - c).wait_recv()

    def event(k, h):
        if k == 0:
            o_copy(h, 1 - c).wait_recv()
            compute([(z, h)])
        else:
            event_wait(k, h)
            compute([(chip(0, k), h), (chip(1, k), h)] if k < 4 else [(chip(0, 4), h)])

    def wp_copy(j):
        to = (wrap(e + j, EP), t)
        return rcopy(wr.at[c, e], wr.at[c, e], s_wp, r_wp, to)

    def wp_all():
        ref = wr.at[c, pl.ds(0, EP - 1)]
        return rcopy(ref, ref, s_wp, r_wp, right)

    def prepare_attention():
        for cp in local[2:6]:
            cp.wait()
        for cp in halo:
            cp.wait_recv()
        q_all().wait_recv()
        k_all().wait_recv()
        local[0].wait()
        kf[:WINDOW] = jnp.where(t == 0, kbuf[2], kbuf[0])
        kf[WINDOW:] = kbuf[1]
        before = jnp.where(t == 0, vbuf[2], vbuf[0]).astype(F32)
        vt[:, :WINDOW] = before.T.astype(BF16)
        vt[:, WINDOW:] = vbuf[1].astype(F32).T.astype(BF16)

    def attend(head):
        token = iota((2 * WINDOW, WINDOW), 1)
        key = iota((2 * WINDOW, WINDOW), 0)
        begin = jnp.where((e == 0) & (t == 0), WINDOW, 0)
        allowed = (key > token) & (key <= token + WINDOW) & (key >= begin)
        scores = mm(kf[...], qz[head]) * HEAD_DIM**-0.5
        masked = jnp.where(allowed, scores, -1e30)
        sink = skrecv[head][0:1, :]
        row_max = jnp.maximum(jnp.max(masked, 0, keepdims=True), sink)
        powers = jnp.where(allowed, jnp.exp(masked - row_max), 0.0)
        sums = jnp.sum(powers, 0, keepdims=True) + jnp.exp(sink - row_max)
        probs = (powers / sums).astype(BF16)
        group = pl.multiple_of((head // 8) * HEAD_DIM, HEAD_DIM)
        place = pl.multiple_of((head // 2) * HEAD_DIM, HEAD_DIM)
        att[lax.rem(head, 2), pl.ds(place, HEAD_DIM)] = mm(vt[pl.ds(group, HEAD_DIM)], probs)

    def turn():
        for i in range(2):
            proj[i] = att[i].T.astype(BF16)

    def x_wait(zb, h):
        x_copy(zb, h).wait_recv()

    def pair_sum(zb, h, col):
        at = pl.ds(h * HALF, HALF)
        cols = slice(col * WIDE, (col + 1) * WIDE)
        return pbuf[zb, at, cols] + inbox[zb, at, cols].astype(F32)

    def rs_copy(direction, k, h, col):
        return rcopy(
            rs_send.at[direction, k - 1, h, col],
            rs_recv.at[direction, k - 1, h, col],
            s_rs,
            r_rs.at[direction, k - 1, h, col],
            ring[direction],
        )

    def rs_go(direction, k, h, col):
        away = LONG[direction][col] + 1 - k
        value = pair_sum(wrap(z + away if direction == 0 else z - away, NZ), h, col)
        if k > 1:
            value = value + rs_recv[direction, k - 2, h, col].astype(F32)
        rs_send[direction, k - 1, h, col] = value.astype(BF16)
        rs_copy(direction, k, h, col).start()

    def rs_begin(h, long):
        for direction in range(2):
            rs_go(direction, 1, h, direction if long else 1 - direction)

    def x_waits(k, h):
        x_wait(chip(0, k), h)
        if 0 < k < 4:
            x_wait(chip(1, k), h)

    def project(lo, hi):
        for i in range(lo, hi):
            out = mm(proj[0], wr[0, i]) + mm(proj[1], wr[1, i])
            mix_ref[:, i * 128 : (i + 1) * 128] = out.astype(BF16)

    def rs_step(k, h, long):
        for direction in range(2):
            col = direction if long else 1 - direction
            if k <= LONG[direction][col]:
                rs_copy(direction, k, h, col).wait_recv()
                if k < LONG[direction][col]:
                    rs_go(direction, k + 1, h, col)

    def b_copy(h, to, frm):
        return rcopy(bsend.at[h, to], brecv.at[h, frm], s_b.at[h], r_b.at[h], (to, t))

    def b_send(h, j):
        b_copy(h, wrap(e + j, EP), e).start()

    def b_all(h):
        rest = slice(0, EP - 1)
        return rcopy(bsend.at[h, rest], brecv.at[h, rest], s_b.at[h], r_b.at[h], right)

    def give_back(h):
        rr = iota((256, HALF), 0)
        good = (iota((256, HALF), 1) == (rr >> 4) * 3 + (rr & 3)) & ((rr & 3) < 3)
        spread_out = None
        for q in range(4):
            col, inner = q // 2, (q % 2) * QUARTER
            value = pair_sum(z, h, col)[:, inner : inner + QUARTER]
            for direction in range(2):
                last = LONG[direction][col] - 1
                value = value + rs_recv[direction, last, h, col, :, inner : inner + QUARTER].astype(F32)
            put = jnp.where(good & (((rr >> 2) & 3) == q), 1.0, 0.0).astype(BF16)
            piece = mm(put, value.astype(BF16))
            spread_out = piece if spread_out is None else spread_out + piece
        bsend[h] = spread_out.astype(BF16).reshape(EP, 16, QUARTER)
        each(1, EP, lambda j: b_send(h, j))
        brecv[h, e] = bsend[h, e]

    wz_step(1)
    launch(0)
    for cp in local[6:]:
        cp.wait()
    event(0, 0)
    launch(1)
    wz_step(2)
    prepare_attention()
    event(0, 1)
    arrival(1, 0, True)
    arrival(1, 0, False)
    arrival(1, 1, True)
    wz_step(3)
    each(0, 4, attend)
    arrival(2, 0, True)
    event(1, 0)
    arrival(2, 0, False)
    arrival(2, 1, True)
    event(2, 0)
    arrival(3, 0, True)
    wz_step(4)
    each(1, EP, lambda j: wp_copy(j).start())
    arrival(3, 0, False)
    arrival(1, 1, False)
    event(3, 0)
    arrival(3, 1, True)
    arrival(4, 0, True)
    each(4, 7, attend)
    x_waits(3, 0)
    rs_begin(0, False)
    arrival(2, 1, False)
    event(4, 0)
    arrival(4, 1, True)
    x_waits(4, 0)
    rs_begin(0, True)
    event(4, 1)
    x_waits(2, 0)
    rs_step(1, 0, False)
    arrival(3, 1, False)
    x_waits(4, 1)
    rs_begin(1, True)
    event(2, 1)
    rs_step(1, 0, True)
    each(7, 10, attend)
    x_waits(1, 0)
    rs_step(2, 0, False)
    event(3, 1)
    x_waits(3, 1)
    rs_step(1, 1, True)
    rs_step(2, 0, True)
    rs_begin(1, False)
    x_waits(2, 1)
    rs_step(2, 1, True)
    each(10, 13, attend)
    rs_step(3, 0, False)
    rs_step(3, 0, True)
    event(1, 1)
    rs_step(1, 1, False)
    x_waits(1, 1)
    rs_step(3, 1, True)
    each(13, 16, attend)
    turn()
    rs_step(4, 0, True)
    x_waits(0, 0)
    wp_all().wait_recv()
    wd_copy = rcopy(wr.at[c], wr.at[c], s_wd, r_wd, partner)
    wd_copy.start()
    give_back(0)
    rs_step(2, 1, False)
    rs_step(4, 1, True)
    rs_step(3, 1, False)
    x_waits(0, 1)
    give_back(1)
    rcopy(wr.at[1 - c], wr.at[1 - c], s_wd, r_wd, partner).wait_recv()
    project(0, 8)
    project(8, 16)

    weight = jnp.where(hit0, rw_ref[0:1, :], 0.0) + jnp.where(hit1, rw_ref[1:2, :], 0.0)
    w_hi = weight.astype(BF16)
    w_lo = (weight - w_hi.astype(F32)).astype(BF16)
    same = jnp.where(iota((32, 32), 0) == iota((32, 32), 1), 1.0, 0.0).astype(BF16)
    parts = [nt(same, mm(expand, part).astype(BF16)) for part in (w_hi, w_lo)]
    quarter = (iota((32, 256), 1) >> 2) & 3
    keep = [nt(same, jnp.where(chosen[h], 1.0, 0.0).astype(BF16)) > 0.5 for h in range(2)]
    for h in range(2):
        b_all(h).wait_recv()
    for q in range(4):
        out = None
        for h in range(2):
            back = brecv[h].reshape(256, QUARTER)
            for part in parts:
                piece = mm(jnp.where(keep[h] & (quarter == q), part, 0.0).astype(BF16), back)
                out = piece if out is None else out + piece
        moe_ref[:, q * QUARTER : (q + 1) * QUARTER] = out.astype(BF16)

    for h in range(2):
        a_all(h).wait_send()
        b_all(h).wait_send()
    q_all().wait_send()
    k_all().wait_send()
    wp_all().wait_send()
    seven = wr.at[c, e, pl.ds(0, (NZ - 1) * HEAD_DIM)]
    rcopy(seven, seven, s_wz, r_wp, right).wait_send()
    for cp in halo:
        cp.wait_send()
    wd_copy.wait_send()
    ring_bytes = agbuf.at[pl.ds(0, 7)]
    for sem in (s_ag, s_d, s_rs):
        rcopy(ring_bytes, ring_bytes, sem, r_wp, right).wait_send()
    rcopy(agbuf.at[t], agbuf.at[t], s_o, r_wp, partner).wait_send()
    rcopy(outbox, inbox, s_x, r_wp, partner).wait_send()


def hand_over(mixed, moved, mix_out, moe_out):
    mix_out[...] = mixed[...]
    moe_out[...] = moved[...]


def body(
    queries,
    key_rows,
    value_rows,
    sink_logits,
    out_weight,
    moe_rows,
    moe_gain,
    routes,
    route_weight,
    gate_weight,
    up_weight,
    down_weight,
):
    vm = pl.BlockSpec(memory_space=pltpu.VMEM)
    hbm = pl.BlockSpec(memory_space=pl.ANY)
    dma = pltpu.SemaphoreType.DMA
    mixed, moved = pl.pallas_call(
        kernel,
        out_shape=(
            jax.ShapeDtypeStruct((WINDOW, D), BF16),
            jax.ShapeDtypeStruct((32, D), BF16),
        ),
        in_specs=[hbm] * 12,
        out_specs=(vm, vm),
        scratch_shapes=[
            pltpu.VMEM((32, D), BF16),
            pltpu.VMEM((1, D), F32),
            pltpu.VMEM((2, 32), jnp.int32),
            pltpu.VMEM((2, 32), F32),
            pltpu.VMEM((1, 1), F32),
            pltpu.VMEM((FF, D), BF16),
            pltpu.VMEM((FF, D), BF16),
            pltpu.VMEM((FF, D), BF16),
            pltpu.VMEM((TPN, HEAD_DIM, WINDOW), BF16),
            pltpu.VMEM((TPN, 2 * HEAD_DIM, WINDOW), BF16),
            pltpu.VMEM((8, 128), F32),
            pltpu.VMEM((TPN, 8, 128), F32),
            pltpu.VMEM((3, WINDOW, 128), BF16),
            pltpu.VMEM((3, WINDOW, 128), BF16),
            pltpu.VMEM((2 * WINDOW, 128), BF16),
            pltpu.VMEM((128, 2 * WINDOW), BF16),
            pltpu.VMEM((2, NZ * HEAD_DIM, WINDOW), F32),
            pltpu.VMEM((2, WINDOW, NZ * HEAD_DIM), BF16),
            pltpu.VMEM((2, EP, NZ * HEAD_DIM, 128), BF16),
            pltpu.VMEM((2, EP, 16, QUARTER), BF16),
            pltpu.VMEM((2, EP, 16, QUARTER), BF16),
            pltpu.VMEM((TPN, ROWS, D), BF16),
            pltpu.VMEM((NZ, ROWS, D), F32),
            pltpu.VMEM((NZ, ROWS, D), BF16),
            pltpu.VMEM((NZ, ROWS, D), BF16),
            pltpu.VMEM((2, 4, 2, 2, HALF, WIDE), BF16),
            pltpu.VMEM((2, 4, 2, 2, HALF, WIDE), BF16),
            pltpu.VMEM((2, EP, 16, QUARTER), BF16),
            pltpu.VMEM((2, EP, 16, QUARTER), BF16),
            dma((14,)),
            dma,
            dma((2,)),
            dma((2,)),
            dma((2,)),
            dma((2,)),
            dma,
            dma,
            dma,
            dma,
            dma((2,)),
            dma((2,)),
            dma,
            dma((2, 4)),
            dma,
            dma,
            dma,
            dma,
            dma,
            dma((2, 4, 2, 2)),
            dma,
            dma((2,)),
            dma,
            dma((2, 4, 2, 2)),
            dma,
            dma((NZ, 2)),
            dma,
            dma((2, 4, 2, 2)),
        ],
        compiler_params=pltpu.CompilerParams(
            collective_id=0, has_side_effects=True, vmem_limit_bytes=60 * 1024 * 1024
        ),
    )(
        moe_rows,
        moe_gain.reshape(1, D),
        routes.T,
        route_weight.T,
        sink_logits.reshape(1, 1),
        queries.T,
        key_rows,
        value_rows,
        out_weight,
        jnp.swapaxes(gate_weight, 1, 2),
        jnp.swapaxes(up_weight, 1, 2),
        down_weight,
    )
    return pl.pallas_call(
        hand_over,
        out_shape=(
            jax.ShapeDtypeStruct((WINDOW, D), BF16),
            jax.ShapeDtypeStruct((32, D), BF16),
        ),
        in_specs=[vm, vm],
        out_specs=(vm, vm),
    )(mixed, moved)


def solution(mesh):
    in_specs = (
        P("ep", "tp"),
        P("ep", None),
        P("ep", None),
        P("tp"),
        P("tp", None),
        P(("ep", "tp"), None),
        P(),
        P(("ep", "tp"), None),
        P(("ep", "tp"), None),
        P("ep", None, "tp"),
        P("ep", None, "tp"),
        P("ep", "tp", None),
    )
    out_specs = (P(("ep", "tp"), None), P(("ep", "tp"), None))
    return jax.shard_map(body, mesh=mesh, in_specs=in_specs, out_specs=out_specs, check_vma=False)
```
